32 devices in a mesh: grp: 2 (over y), fs: 4 (over z), tp: 4 (over x, core).
Axes of the slice: x: 2, y: 2, z: 4, core: 2. Of those that a mesh axis runs over, the one named last changes fastest.
Arguments:
- stream: bfloat16 [2048, 3072], P('tp', ('grp', 'fs')), parts along dimension 1, may hold values from -6 to 6
- mixer_gain: float32 [2048], replicated, may hold values from 0.1 to 1.9
- glu_value: bfloat16 [2048, 1024], P('fs', 'tp'), may hold values from -0.125 to 0.125
- glu_gate: bfloat16 [2048, 1024], P('fs', 'tp'), may hold values from -0.125 to 0.125
- conv_kernel: bfloat16 [31, 1024], replicated, may hold values from -1 to 1
- channel_gain: float32 [1024], replicated, may hold values from 0.1 to 1.9
- conv_out: bfloat16 [2048, 1024], P('fs', 'tp'), may hold values from -0.1875 to 0.1875
- ffn_gain: float32 [2048], replicated, may hold values from 0.1 to 1.9
- ffn_gate: bfloat16 [2048, 5632], P('fs', 'tp'), may hold values from -0.125 to 0.125
- ffn_up: bfloat16 [2048, 5632], P('fs', 'tp'), may hold values from -0.125 to 0.125
- ffn_down: bfloat16 [2048, 5632], P('fs', 'tp'), may hold values from -0.078125 to 0.078125
Outputs:
- result: bfloat16 [2048, 3072], P('tp', ('grp', 'fs')), parts along dimension 1
The draws below stay inside these ranges and needn't reach their ends.
There are 2 independent parts, one for each index of `grp`. The reference program is written for one: setup_inputs(seed, part) draws one part's arguments, and reference() takes and returns one part's arrays. A program takes and returns all parts, laid end to end along the dimension named above; an argument that names none is the same for every part. Nothing has to cross between parts.
All inputs are finite; a program needn't handle non-finite values.
Results may differ from the reference program's by a relative error of at most 0.018.
Values may be sent and summed in bfloat16 or wider, within the bound.
A program may use at most 64 MiB of HBM per device.

```python
import jax
import jax.numpy as jnp
from jax import lax

D = 2048
DC = 1024
FF = 5632
KERNEL = 31
TOK_DEV = 384
TOKENS = 1536
N_TP = 4


def steps_of(stream_key, shape, pieces, low, largest):
    level, own = 1.0, jax.random.fold_in(stream_key, 6)
    for dim, blocks in pieces:
        steps = jnp.exp(jax.random.uniform(jax.random.fold_in(own, dim), (blocks,), jnp.float32, low / len(pieces), largest / len(pieces)))
        level = level * jnp.repeat(steps, shape[dim] // blocks).reshape([-1 if axis == dim else 1 for axis in range(len(shape))])
    return level


def bell_draw(rng, shape, deviation, limit, pieces=(), kind=jnp.bfloat16):
    entries = jax.random.normal(rng, shape, jnp.float32) * deviation
    if len(pieces) > 0:
        entries = steps_of(rng, shape, pieces, -0.22, 0.18) * entries
    return jnp.clip(entries, min=-limit, max=limit).astype(kind)


def setup_inputs(seed: int = 0, part: int = 0) -> dict:
    splits = jax.random.split(jax.random.key(seed), 12)
    part_keys = jax.random.split(jax.random.fold_in(splits[11], part), 12)
    return {
        "stream": bell_draw(part_keys[0], (D, TOKENS), 1.0, 6.0, ((0, 4), (1, 4))),
        "mixer_gain": jnp.clip(1.0 + 0.18 * jax.random.normal(splits[1], (D,), jnp.float32), 0.1, 1.9),
        "glu_value": bell_draw(splits[2], (D, DC), D ** -0.5, 0.125, ((0, 4), (1, 4))),
        "glu_gate": bell_draw(splits[3], (D, DC), D ** -0.5, 0.125, ((0, 4), (1, 4))),
        "conv_kernel": bell_draw(splits[4], (KERNEL, DC), KERNEL ** -0.5, 1.0),
        "channel_gain": jnp.clip(1.0 + 0.18 * jax.random.normal(splits[5], (DC,), jnp.float32), 0.1, 1.9),
        "conv_out": bell_draw(splits[6], (D, DC), DC ** -0.5, 0.1875, ((0, 4), (1, 4))),
        "ffn_gain": jnp.clip(1.0 + 0.18 * jax.random.normal(splits[7], (D,), jnp.float32), 0.1, 1.9),
        "ffn_gate": bell_draw(splits[8], (D, FF), D ** -0.5, 0.125, ((0, 4), (1, 4))),
        "ffn_up": bell_draw(splits[9], (D, FF), D ** -0.5, 0.125, ((0, 4), (1, 4))),
        "ffn_down": bell_draw(splits[10], (D, FF), FF ** -0.5, 0.078125, ((0, 4), (1, 4))),
    }


def rms_normalize(wide, gain):
    inverse = lax.rsqrt(lax.optimization_barrier(jnp.mean(wide * wide, axis=0, keepdims=True)) + 1e-06)
    return (wide * inverse * gain[:, None]).astype(jnp.bfloat16)

def block_sums(weight, acts):
    total_rows = weight.shape[0]
    width = weight.shape[1]
    length = acts.shape[1]
    blocked_w = weight.reshape(total_rows, N_TP, width // N_TP).astype(jnp.float32)
    blocked_a = acts.reshape(N_TP, width // N_TP, length).astype(jnp.float32)
    partials = jnp.einsum('dpc,pcl->pdl', blocked_w, blocked_a)
    rounded = lax.optimization_barrier(partials.astype(jnp.bfloat16))
    return lax.optimization_barrier(jnp.sum(rounded.astype(jnp.float32), axis=0))

def one_sequence(seq, mixer_gain, glu_value, glu_gate, conv_kernel, channel_gain, conv_out, ffn_gain, ffn_gate, ffn_up, ffn_down):
    length = seq.shape[1]
    wide = seq.astype(jnp.float32)
    normed = rms_normalize(wide, mixer_gain)
    value_part = jnp.dot(glu_value.T, normed, preferred_element_type=jnp.float32)
    gate_part = jnp.dot(glu_gate.T, normed, preferred_element_type=jnp.float32)
    gated = (value_part * jax.nn.sigmoid(gate_part)).astype(jnp.float32)
    gated = lax.optimization_barrier(gated.astype(jnp.bfloat16)).astype(jnp.float32)
    padded = jnp.pad(gated, ((0, 0), (KERNEL - 1, 0)))
    taps = conv_kernel.astype(jnp.float32)
    conv_sum = jnp.zeros_like(gated)
    for step in range(KERNEL):
        conv_sum = conv_sum + taps[step][:, None] * padded[:, step:step + length]
    mean_val = lax.optimization_barrier(jnp.mean(conv_sum, axis=0, keepdims=True))
    mean_sq = lax.optimization_barrier(jnp.mean(conv_sum * conv_sum, axis=0, keepdims=True))
    scaled = (conv_sum - mean_val) * lax.rsqrt(mean_sq - mean_val * mean_val + 1e-05) * channel_gain[:, None]
    activated = jax.nn.silu(scaled).astype(jnp.bfloat16)
    mixed_sum = block_sums(conv_out, activated)
    middle = (wide + mixed_sum).astype(jnp.bfloat16)
    middle_wide = middle.astype(jnp.float32)
    normed_two = rms_normalize(middle_wide, ffn_gain)
    gate_val = jnp.dot(ffn_gate.T, normed_two, preferred_element_type=jnp.float32)
    up_val = jnp.dot(ffn_up.T, normed_two, preferred_element_type=jnp.float32)
    hidden = (jax.nn.silu(gate_val) * up_val).astype(jnp.bfloat16)
    ffn_sum = block_sums(ffn_down, hidden)
    return (middle_wide + ffn_sum).astype(jnp.bfloat16)

def reference(stream, mixer_gain, glu_value, glu_gate, conv_kernel, channel_gain, conv_out, ffn_gain, ffn_gate, ffn_up, ffn_down):
    width = stream.shape[0]
    count = stream.shape[1] // TOK_DEV
    seqs = jnp.transpose(stream.reshape(width, count, TOK_DEV), (1, 0, 2))

    def run(seq):
        return one_sequence(seq, mixer_gain, glu_value, glu_gate, conv_kernel, channel_gain, conv_out, ffn_gain, ffn_gate, ffn_up, ffn_down)
    outputs = lax.map(run, seqs)
    return jnp.transpose(outputs, (1, 0, 2)).reshape(width, count * TOK_DEV)
```

```python
import functools

import jax
import jax.numpy as jnp
from jax import lax
from jax.experimental import pallas as pl
from jax.experimental.pallas import tpu as pltpu
from jax.sharding import PartitionSpec as P

MESH = pl.DeviceIdType.MESH
NT = (((1,), (1,)), ((), ()))
FIRST = 4


def layer_kernel(
    n_grp, n_fs, n_tp, pieces, total_channels,
    stream, w0, w1, w2, w3, w4, w5,
    mixer_gain, conv_kernel, channel_gain, ffn_gain,
    out,
    b0, b1, b2, b3, b4, b5,
    x_all, x_wide, x_norm, padded, stat_out, stat_in,
    part_one, got_one, middle_all, acc, hidden, part_two, got_two,
    z_recv, y_recv, left_send, right_send, y_send, own_sem,
    x_recv, x_send, st_recv, st_send,
    p1_recv, p1_send, m_recv, m_send, p2_recv, p2_send,
):
    y = lax.axis_index("grp")
    f = lax.axis_index("fs")
    t = lax.axis_index("tp")
    weights = (w0, w1, w2, w3, w4, w5)
    bufs = (b0, b1, b2, b3, b4, b5)
    feats, length = stream.shape
    width = feats * n_tp
    per = n_fs // n_tp
    rows = width // n_fs

    def tp_peer(k):
        return lax.rem(t + k, n_tp)

    barrier = pltpu.get_barrier_semaphore()
    for k in range(1, n_tp):
        pl.semaphore_signal(barrier, inc=1, device_id={"tp": tp_peer(k)}, device_id_type=MESH)
    for k in range(1, n_grp):
        pl.semaphore_signal(
            barrier, inc=1, device_id={"grp": lax.rem(y + k, n_grp)}, device_id_type=MESH
        )

    @pl.when(f > 0)
    def _():
        pl.semaphore_signal(barrier, inc=1, device_id={"fs": f - 1}, device_id_type=MESH)

    @pl.when(f < n_fs - 1)
    def _():
        pl.semaphore_signal(barrier, inc=1, device_id={"fs": f + 1}, device_id_type=MESH)

    ends = (f + n_fs - 1) // n_fs + (2 * (n_fs - 1) - f) // n_fs
    pl.semaphore_wait(barrier, n_tp - 1 + n_grp - 1 + ends)

    def remote(src, dst, send, recv, where):
        return pltpu.make_async_remote_copy(
            src_ref=src, dst_ref=dst, send_sem=send, recv_sem=recv,
            device_id=where, device_id_type=MESH,
        )

    def slot(c, s, half):
        w, u, subs = pieces[c]
        return bufs[w].at[s, half * subs + u]

    def own_src(c):
        w, u, subs = pieces[c]
        size = bufs[w].shape[2]
        start = pl.multiple_of((y * subs + u) * size, size)
        return weights[w].at[pl.ds(start, size)]

    def z_copy(c, s, step, src=None):
        here = slot(c, s, y)
        sems = right_send if step > 0 else left_send
        return remote(
            here if src is None else src, here, sems.at[c, s], z_recv.at[c, s], {"fs": f + step}
        )

    def y_copy(c, s, half):
        here = slot(c, s, half)
        return remote(
            here, here, y_send.at[c, s], y_recv.at[c, s], {"grp": lax.rem(y + 1, n_grp)}
        )

    def send_own(c):
        @pl.when(f > 0)
        def _():
            z_copy(c, f, -1, own_src(c)).start()

        @pl.when(f < n_fs - 1)
        def _():
            z_copy(c, f, 1, own_src(c)).start()

    def each_distance(body):
        if n_fs <= 4:
            for d in range(1, n_fs):
                body(d)
        else:
            lax.fori_loop(1, n_fs, lambda d, carry: (body(d), carry)[1], 0)

    def forward(c, d):
        @pl.when(f - d >= 0)
        def _():
            s = jnp.maximum(f - d, 0)
            z_copy(c, s, 1).wait_recv()

            @pl.when(f < n_fs - 1)
            def _():
                z_copy(c, s, 1).start()

            y_copy(c, s, y).start()

        @pl.when(f + d < n_fs)
        def _():
            s = jnp.minimum(f + d, n_fs - 1)
            z_copy(c, s, -1).wait_recv()

            @pl.when(f > 0)
            def _():
                z_copy(c, s, -1).start()

            y_copy(c, s, y).start()

    def other_half(c, s):
        y_copy(c, s, lax.rem(y + 1, n_grp)).wait_recv()

    def other_halves(cs, d):
        @pl.when(f - d >= 0)
        def _():
            for c in cs:
                other_half(c, jnp.maximum(f - d, 0))

        @pl.when(f + d < n_fs)
        def _():
            for c in cs:
                other_half(c, jnp.minimum(f + d, n_fs - 1))

    count = len(pieces)
    of = [[c for c in range(count) if pieces[c][0] == w] for w in range(6)]
    glue = of[0] + of[1] + of[2]

    x_copies = []
    for k in range(1, n_tp):
        x_copies.append(
            remote(stream, x_all.at[t], x_send.at[k], x_recv.at[t], {"tp": tp_peer(k)})
        )
        x_copies[-1].start()
    for c in range(FIRST):
        send_own(c)
    x_own = pltpu.make_async_copy(stream, x_all.at[t], own_sem.at[0])
    x_own.start()
    owns = []
    for w in range(6):
        parts, size = bufs[w].shape[1], bufs[w].shape[2]
        for p in range(parts):
            owns.append(
                pltpu.make_async_copy(
                    weights[w].at[pl.ds(p * size, size)], bufs[w].at[f, p],
                    own_sem.at[1 + len(owns)],
                )
            )
            owns[-1].start()
    padded[pl.ds(0, 32), :] = jnp.zeros((32, padded.shape[1]), jnp.float32)

    def normalize(source, gain):
        for start in range(0, length, 128):
            tokens = pl.ds(start, 128)
            total = jnp.zeros((128, 1), jnp.float32)
            for b in range(n_tp):
                block = source[b, :, tokens].astype(jnp.float32).T
                x_wide[b, tokens, :] = block
                total = total + jnp.sum(block * block, axis=1, keepdims=True)
            inverse = lax.rsqrt(total / width + 1e-06)
            for b in range(n_tp):
                scaled = x_wide[b, tokens, :] * inverse * gain[:, pl.ds(b * feats, feats)]
                scaled = scaled.astype(jnp.bfloat16)
                for j in range(per):
                    x_norm[b * per + j, tokens, :] = scaled[:, j * rows : (j + 1) * rows]

    def weight_block(w, s, columns):
        block = bufs[w][s, :, :, columns]
        return block.reshape(rows, block.shape[-1])

    for c in glue:
        forward(c, 1)
    for k in range(1, n_tp):
        src = tp_peer(k)
        remote(
            stream, x_all.at[src], x_send.at[k], x_recv.at[src], {"tp": src}
        ).wait_recv()
    x_own.wait()
    normalize(x_all, mixer_gain)

    def rest(d):
        for c in glue:
            forward(c, d)

    if n_fs <= 4:
        for d in range(2, n_fs):
            rest(d)
    else:
        lax.fori_loop(2, n_fs, lambda d, carry: (rest(d), carry)[1], 0)
    for c in range(FIRST, count):
        send_own(c)
    forward(of[3][0], 1)
    for copy in owns:
        copy.wait()
    each_distance(lambda d: other_halves(of[0] + of[1], d))

    channels = w0.shape[1]
    everything = pl.ds(0, channels)

    def project(w, columns):
        def add(s, total):
            return total + jnp.dot(
                x_norm[s], weight_block(w, s, columns), preferred_element_type=jnp.float32
            )

        return lax.fori_loop(0, n_fs, add, jnp.zeros((length, columns.size), jnp.float32))

    value_part = project(0, everything)
    gate_part = project(1, everything)
    gated = (value_part * jax.nn.sigmoid(gate_part)).astype(jnp.bfloat16)
    padded[pl.ds(32, length), :] = gated.astype(jnp.float32)

    mine = pl.ds(pl.multiple_of(t * channels, channels), channels)
    taps = conv_kernel[:, mine].astype(jnp.float32)
    n_taps = conv_kernel.shape[0]
    lane = lax.broadcasted_iota(jnp.int32, (128, 128), 1)
    conv = []
    for start in range(0, length, 128):
        total = jnp.zeros((128, channels), jnp.float32)
        for k in range(n_taps):
            total = total + taps[k : k + 1, :] * padded[
                pl.ds(start + 32 - (n_taps - 1) + k, 128), :
            ]
        conv.append(total)
        sums = jnp.sum(total, axis=1, keepdims=True)
        squares = jnp.sum(total * total, axis=1, keepdims=True)
        both = jnp.where(lane == 0, sums, jnp.where(lane == 1, squares, 0.0))
        stat_out[:, pl.ds(start, 128)] = both.T[:8, :]

    for k in range(1, n_tp):
        remote(
            stat_out, stat_in.at[t], st_send.at[k], st_recv.at[t], {"tp": tp_peer(k)}
        ).start()
    for c in of[3]:
        if c != of[3][0]:
            forward(c, 1)
    each_distance(lambda d: other_halves(of[2], d))
    for k in range(1, n_tp):
        src = tp_peer(k)
        remote(
            stat_out, stat_in.at[src], st_send.at[k], st_recv.at[src], {"tp": src}
        ).wait_recv()
    stats = stat_out[...]
    for k in range(1, n_tp):
        stats = stats + stat_in[tp_peer(k)]
    activated = []
    for i, start in enumerate(range(0, length, 128)):
        turned = jnp.concatenate(
            [stats[:, start : start + 128], jnp.zeros((120, 128), jnp.float32)], axis=0
        ).T
        mean_val = turned[:, 0:1] / total_channels
        mean_sq = turned[:, 1:2] / total_channels
        scaled = (
            (conv[i] - mean_val)
            * lax.rsqrt(mean_sq - mean_val * mean_val + 1e-05)
            * channel_gain[:, mine]
        )
        activated.append(jax.nn.silu(scaled).astype(jnp.bfloat16))
    activated = jnp.concatenate(activated, axis=0)

    def share(part, got, p_send, p_recv, s):
        dest = s // per
        return remote(
            part.at[s], got.at[t, lax.rem(s, per)], p_send.at[s],
            p_recv.at[t, lax.rem(s, per)], {"tp": dest},
        )

    def send_share(part, got, p_send, p_recv, s):
        @pl.when(s // per != t)
        def _():
            share(part, got, p_send, p_recv, s).start()

    def collect(part, got, p_send, p_recv, base, store):
        for k in range(1, n_tp):
            src = tp_peer(k)
            for j in range(per):
                remote(
                    part.at[j], got.at[src, j], p_send.at[j], p_recv.at[src, j], {"tp": src}
                ).wait_recv()
        for j in range(per):
            here = pl.ds(j * rows, rows)
            total = part[t * per + j].astype(jnp.float32)
            for k in range(1, n_tp):
                total = total + got[tp_peer(k), j].astype(jnp.float32)
            store(here, base[here, :].astype(jnp.float32) + total)

    def mix(s, carry):
        part_one[s] = lax.dot_general(
            weight_block(2, s, everything), activated, NT, preferred_element_type=jnp.float32
        ).astype(jnp.bfloat16)
        send_share(part_one, got_one, p1_send, p1_recv, s)
        return carry

    lax.fori_loop(0, n_fs, mix, 0)

    def many(cs, first, last):
        def go(d):
            for c in cs:
                forward(c, d)

        if n_fs <= 4:
            for d in range(first, last):
                go(d)
        else:
            lax.fori_loop(first, last, lambda d, carry: (go(d), carry)[1], 0)

    many(of[3], 2, n_fs - 1)

    def keep_middle(here, value):
        middle_all[t, here, :] = value.astype(jnp.bfloat16)

    collect(part_one, got_one, p1_send, p1_recv, x_all.at[t], keep_middle)
    for k in range(1, n_tp):
        remote(
            middle_all.at[t], middle_all.at[t], m_send.at[k], m_recv.at[t], {"tp": tp_peer(k)}
        ).start()
    many(of[3], n_fs - 1, n_fs)
    for c in of[4]:
        forward(c, 1)
    for k in range(1, n_tp):
        src = tp_peer(k)
        remote(
            middle_all.at[src], middle_all.at[src], m_send.at[k], m_recv.at[src], {"tp": src}
        ).wait_recv()
    normalize(middle_all, ffn_gain)
    many(of[4], 2, n_fs - 1)
    each_distance(lambda d: other_halves(of[3], d))

    units = w3.shape[1]
    tiles = [pl.ds(a, min(256, units - a)) for a in range(0, units, 256)]
    for columns in tiles:
        acc[:, columns] = project(3, columns)
    many(of[4], n_fs - 1, n_fs)
    for c in of[5]:
        forward(c, 1)
    each_distance(lambda d: other_halves(of[4], d))
    for columns in tiles:
        hidden[:, columns] = (jax.nn.silu(acc[:, columns]) * project(4, columns)).astype(
            jnp.bfloat16
        )

    def down(s):
        block = bufs[5][s].reshape(rows, units)
        part_two[s] = lax.dot_general(
            block, hidden[...], NT, preferred_element_type=jnp.float32
        ).astype(jnp.bfloat16)
        send_share(part_two, got_two, p2_send, p2_recv, s)

    def down_at(d):
        other_halves(of[5], d)

        def both(i, carry):
            s = f + d - 2 * d * i

            @pl.when(jnp.logical_and(s >= 0, s < n_fs))
            def _():
                down(jnp.clip(s, 0, n_fs - 1))

            return carry

        lax.fori_loop(0, 2, both, 0)

    down(f)

    def last(d):
        for c in of[5]:
            forward(c, d)
        down_at(d - 1)

    if n_fs <= 4:
        for d in range(2, n_fs):
            last(d)
    else:
        lax.fori_loop(2, n_fs, lambda d, carry: (last(d), carry)[1], 0)
    down_at(n_fs - 1)

    def keep_result(here, value):
        out[here, :] = value.astype(jnp.bfloat16)

    collect(part_two, got_two, p2_send, p2_recv, middle_all.at[t], keep_result)

    for copy in x_copies:
        copy.wait_send()
    for k in range(1, n_tp):
        remote(
            stat_out, stat_in.at[t], st_send.at[k], st_recv.at[t], {"tp": tp_peer(k)}
        ).wait_send()
        remote(
            middle_all.at[t], middle_all.at[t], m_send.at[k], m_recv.at[t], {"tp": tp_peer(k)}
        ).wait_send()

    def drain(s, carry):
        @pl.when(s // per != t)
        def _():
            share(part_one, got_one, p1_send, p1_recv, s).wait_send()
            share(part_two, got_two, p2_send, p2_recv, s).wait_send()

        for c in range(count):
            @pl.when(jnp.logical_and(s <= f, f < n_fs - 1))
            def _():
                z_copy(c, s, 1).wait_send()

            @pl.when(jnp.logical_and(s >= f, f > 0))
            def _():
                z_copy(c, s, -1).wait_send()

            @pl.when(s != f)
            def _():
                y_copy(c, s, y).wait_send()

        return carry

    lax.fori_loop(0, n_fs, drain, 0)


def on_device(sizes, *args):
    (stream, mixer_gain, glu_value, glu_gate, conv_kernel, channel_gain,
     conv_out, ffn_gain, ffn_gate, ffn_up, ffn_down) = args
    n_grp, n_fs, n_tp = sizes
    weights = (glu_value, glu_gate, conv_out, ffn_gate, ffn_up, ffn_down)
    feats, length = stream.shape
    width = feats * n_tp
    rows = width // n_fs
    channels = glu_value.shape[1]
    units = ffn_gate.shape[1]
    pieces, bufs = [], []
    for w, weight in enumerate(weights):
        subs = 2 if (w >= 3 and n_fs <= 4) else 1
        pieces += [(w, u, subs) for u in range(subs)]
        bufs.append(
            pltpu.VMEM(
                (n_fs, n_grp * subs, rows // (n_grp * subs), weight.shape[1]), jnp.bfloat16
            )
        )
    count = len(pieces)
    per = n_fs // n_tp
    any_spec = pl.BlockSpec(memory_space=pl.ANY)
    vmem = pl.BlockSpec(memory_space=pltpu.VMEM)
    dma = pltpu.SemaphoreType.DMA
    owns = 1 + sum(buf.shape[1] for buf in bufs)
    return pl.pallas_call(
        functools.partial(
            layer_kernel, n_grp, n_fs, n_tp, tuple(pieces), channel_gain.shape[0]
        ),
        out_shape=jax.ShapeDtypeStruct((feats, length), jnp.bfloat16),
        in_specs=[any_spec] * 7 + [vmem] * 4,
        out_specs=vmem,
        scratch_shapes=bufs
        + [
            pltpu.VMEM((n_tp, feats, length), jnp.bfloat16),
            pltpu.VMEM((n_tp, length, feats), jnp.float32),
            pltpu.VMEM((n_fs, length, rows), jnp.bfloat16),
            pltpu.VMEM((length + 32, channels), jnp.float32),
            pltpu.VMEM((8, length), jnp.float32),
            pltpu.VMEM((n_tp, 8, length), jnp.float32),
            pltpu.VMEM((n_fs, rows, length), jnp.bfloat16),
            pltpu.VMEM((n_tp, per, rows, length), jnp.bfloat16),
            pltpu.VMEM((n_tp, feats, length), jnp.bfloat16),
            pltpu.VMEM((length, units), jnp.float32),
            pltpu.VMEM((length, units), jnp.bfloat16),
            pltpu.VMEM((n_fs, rows, length), jnp.bfloat16),
            pltpu.VMEM((n_tp, per, rows, length), jnp.bfloat16),
        ]
        + [dma((count, n_fs))] * 5
        + [dma((owns,))]
        + [dma((n_tp,))] * 4
        + [dma((n_tp, per)), dma((n_fs,))]
        + [dma((n_tp,))] * 2
        + [dma((n_tp, per)), dma((n_fs,))],
        compiler_params=pltpu.CompilerParams(
            collective_id=0, has_side_effects=True, vmem_limit_bytes=62 * 1024 * 1024
        ),
    )(
        stream, *weights, mixer_gain[None, :], conv_kernel, channel_gain[None, :],
        ffn_gain[None, :],
    )


def solution(mesh):
    in_specs = (
        P("tp", ("grp", "fs")),
        P(),
        P("fs", "tp"),
        P("fs", "tp"),
        P(),
        P(),
        P("fs", "tp"),
        P(),
        P("fs", "tp"),
        P("fs", "tp"),
        P("fs", "tp"),
    )
    sizes = (mesh.shape["grp"], mesh.shape["fs"], mesh.shape["tp"])
    return jax.shard_map(
        functools.partial(on_device, sizes), mesh=mesh, in_specs=in_specs,
        out_specs=P("tp", ("grp", "fs")), check_vma=False,
    )
```

```python
import functools

import jax
import jax.numpy as jnp
from jax import lax
from jax.experimental import pallas as pl
from jax.experimental.pallas import tpu as pltpu
from jax.sharding import PartitionSpec as P

MESH = pl.DeviceIdType.MESH
NT = (((1,), (1,)), ((), ()))
FIRST = 4


def layer_kernel(
    n_grp, n_fs, n_tp, pieces, total_channels,
    stream, w0, w1, w2, w3, w4, w5,
    mixer_gain, conv_kernel, channel_gain, ffn_gain,
    out,
    b0, b1, b2, b3, b4, b5,
    x_all, x_wide, x_norm, padded, stat_out, stat_in,
    part_one, got_one, middle_all, acc, hidden, part_two, got_two,
    returned, back,
    z_recv, y_recv, left_send, right_send, y_send, own_sem, g_sem,
    x_recv, x_send, st_recv, st_send,
    p1_recv, p1_send, m_recv, m_send, p2_recv, p2_send,
):
    y = lax.axis_index("grp")
    f = lax.axis_index("fs")
    t = lax.axis_index("tp")
    weights = (w0, w1, w2, w3, w4, w5)
    bufs = (b0, b1, b2, b3, b4, b5)
    feats, length = stream.shape
    width = feats * n_tp
    per = n_fs // n_tp
    rows = width // n_fs

    inner = jnp.logical_and(f > 0, f < n_fs - 1)
    guest = jnp.logical_or(f == 1, f == n_fs - 2)
    toward = jnp.where(f == 0, 1, -1)

    def tp_peer(k):
        return lax.rem(t + k, n_tp)

    barrier = pltpu.get_barrier_semaphore()
    for k in range(1, n_tp):
        pl.semaphore_signal(barrier, inc=1, device_id={"tp": tp_peer(k)}, device_id_type=MESH)
    for k in range(1, n_grp):
        pl.semaphore_signal(
            barrier, inc=1, device_id={"grp": lax.rem(y + k, n_grp)}, device_id_type=MESH
        )

    @pl.when(f > 0)
    def _():
        pl.semaphore_signal(barrier, inc=1, device_id={"fs": f - 1}, device_id_type=MESH)

    @pl.when(f < n_fs - 1)
    def _():
        pl.semaphore_signal(barrier, inc=1, device_id={"fs": f + 1}, device_id_type=MESH)

    ends = (f + n_fs - 1) // n_fs + (2 * (n_fs - 1) - f) // n_fs
    pl.semaphore_wait(barrier, n_tp - 1 + n_grp - 1 + ends)

    def remote(src, dst, send, recv, where):
        return pltpu.make_async_remote_copy(
            src_ref=src, dst_ref=dst, send_sem=send, recv_sem=recv,
            device_id=where, device_id_type=MESH,
        )

    def slot(c, s, half):
        w, u, subs = pieces[c]
        return bufs[w].at[s, half * subs + u]

    def is_ffn(c):
        return pieces[c][0] >= 3

    def own_src(c, half):
        w, u, subs = pieces[c]
        size = bufs[w].shape[2]
        start = pl.multiple_of((half * subs + u) * size, size)
        return weights[w].at[pl.ds(start, size)]

    def z_copy(c, s, step, src=None):
        here = slot(c, s, y)
        sems = right_send if step > 0 else left_send
        return remote(
            here if src is None else src, here, sems.at[c, s], z_recv.at[c, s], {"fs": f + step}
        )

    def other_y():
        return lax.rem(y + 1, n_grp)

    def z_extra(c, step):
        return remote(
            own_src(c, other_y()), slot(c, f, other_y()), y_send.at[c, f], y_recv.at[c, f],
            {"fs": f + step},
        )

    def y_copy(c, s, half):
        here = slot(c, s, half)
        return remote(here, here, y_send.at[c, s], y_recv.at[c, s], {"grp": other_y()})

    def goes_left(c):
        return f > (1 if is_ffn(c) else 0)

    def goes_right(c):
        return f < (n_fs - 2 if is_ffn(c) else n_fs - 1)

    def send_own(c):
        @pl.when(goes_left(c))
        def _():
            z_copy(c, f, -1, own_src(c, y)).start()

        @pl.when(goes_right(c))
        def _():
            z_copy(c, f, 1, own_src(c, y)).start()

        if is_ffn(c):
            @pl.when(f == 0)
            def _():
                z_extra(c, 1).start()

            @pl.when(f == n_fs - 1)
            def _():
                z_extra(c, -1).start()

    def each_distance(body):
        if n_fs <= 4:
            for d in range(1, n_fs):
                body(d)
        else:
            lax.fori_loop(1, n_fs, lambda d, carry: (body(d), carry)[1], 0)

    def by_y(c, s):
        if not is_ffn(c):
            return s != f
        near = jnp.logical_or(
            jnp.logical_and(s == 0, f == 1), jnp.logical_and(s == n_fs - 1, f == n_fs - 2)
        )
        return jnp.logical_and(jnp.logical_and(inner, s != f), jnp.logical_not(near))

    def forward(c, d):
        from_left, from_right = f - d >= 0, f + d < n_fs
        if is_ffn(c):
            from_left = jnp.logical_and(from_left, inner)
            from_right = jnp.logical_and(from_right, inner)

        @pl.when(from_left)
        def _():
            s = jnp.maximum(f - d, 0)
            z_copy(c, s, 1).wait_recv()

            @pl.when(goes_right(c))
            def _():
                z_copy(c, s, 1).start()

            @pl.when(by_y(c, s))
            def _():
                y_copy(c, s, y).start()

        @pl.when(from_right)
        def _():
            s = jnp.minimum(f + d, n_fs - 1)
            z_copy(c, s, -1).wait_recv()

            @pl.when(goes_left(c))
            def _():
                z_copy(c, s, -1).start()

            @pl.when(by_y(c, s))
            def _():
                y_copy(c, s, y).start()

    def other_half(c, s):
        y_copy(c, s, other_y()).wait_recv()

    def other_halves(cs, d):
        @pl.when(f - d >= 0)
        def _():
            for c in cs:
                other_half(c, jnp.maximum(f - d, 0))

        @pl.when(f + d < n_fs)
        def _():
            for c in cs:
                other_half(c, jnp.minimum(f + d, n_fs - 1))

    count = len(pieces)
    of = [[c for c in range(count) if pieces[c][0] == w] for w in range(6)]
    glue = of[0] + of[1] + of[2]

    x_copies = []
    for k in range(1, n_tp):
        x_copies.append(
            remote(stream, x_all.at[t], x_send.at[k], x_recv.at[t], {"tp": tp_peer(k)})
        )
        x_copies[-1].start()
    for c in range(FIRST):
        send_own(c)
    x_own = pltpu.make_async_copy(stream, x_all.at[t], own_sem.at[0])
    x_own.start()
    owns, ffn_owns = [], []
    for w in range(6):
        parts, size = bufs[w].shape[1], bufs[w].shape[2]
        for p in range(parts):
            kept = owns if w < 3 else ffn_owns
            kept.append(
                pltpu.make_async_copy(
                    weights[w].at[pl.ds(p * size, size)], bufs[w].at[f, p],
                    own_sem.at[1 + len(owns) + len(ffn_owns)],
                )
            )
    for copy in owns:
        copy.start()

    @pl.when(inner)
    def _():
        for copy in ffn_owns:
            copy.start()

    padded[pl.ds(0, 32), :] = jnp.zeros((32, padded.shape[1]), jnp.float32)

    def normalize(source, gain, base=0):
        for start in range(0, length, 128):
            tokens = pl.ds(start, 128)
            total = jnp.zeros((128, 1), jnp.float32)
            for b in range(n_tp):
                block = source[b, :, tokens].astype(jnp.float32).T
                x_wide[b, tokens, :] = block
                total = total + jnp.sum(block * block, axis=1, keepdims=True)
            inverse = lax.rsqrt(total / width + 1e-06)
            for b in range(n_tp):
                scaled = x_wide[b, tokens, :] * inverse * gain[:, pl.ds(b * feats, feats)]
                scaled = scaled.astype(jnp.bfloat16)
                for j in range(per):
                    x_norm[b * per + j, pl.ds(base + start, 128), :] = scaled[:, j * rows : (j + 1) * rows]

    def weight_block(w, s, columns):
        block = bufs[w][s, :, :, columns]
        return block.reshape(rows, block.shape[-1])

    for c in glue:
        forward(c, 1)
    for k in range(1, n_tp):
        src = tp_peer(k)
        remote(
            stream, x_all.at[src], x_send.at[k], x_recv.at[src], {"tp": src}
        ).wait_recv()
    x_own.wait()
    normalize(x_all, mixer_gain)

    def rest(d):
        for c in glue:
            forward(c, d)

    if n_fs <= 4:
        for d in range(2, n_fs):
            rest(d)
    else:
        lax.fori_loop(2, n_fs, lambda d, carry: (rest(d), carry)[1], 0)
    for c in range(FIRST, count):
        if pieces[c][0] < 5:
            send_own(c)
        else:
            @pl.when(inner)
            def _():
                send_own(c)
    forward(of[3][0], 1)
    for copy in owns:
        copy.wait()
    each_distance(lambda d: other_halves(of[0] + of[1], d))

    channels = w0.shape[1]
    everything = pl.ds(0, channels)

    def project(w, columns, base=0):
        def add(s, total):
            return total + jnp.dot(
                x_norm[s, pl.ds(base, length), :], weight_block(w, s, columns), preferred_element_type=jnp.float32
            )

        return lax.fori_loop(0, n_fs, add, jnp.zeros((length, columns.size), jnp.float32))

    value_part = project(0, everything)
    gate_part = project(1, everything)
    gated = (value_part * jax.nn.sigmoid(gate_part)).astype(jnp.bfloat16)
    padded[pl.ds(32, length), :] = gated.astype(jnp.float32)

    mine = pl.ds(pl.multiple_of(t * channels, channels), channels)
    taps = conv_kernel[:, mine].astype(jnp.float32)
    n_taps = conv_kernel.shape[0]
    lane = lax.broadcasted_iota(jnp.int32, (128, 128), 1)
    conv = []
    for start in range(0, length, 128):
        total = jnp.zeros((128, channels), jnp.float32)
        for k in range(n_taps):
            total = total + taps[k : k + 1, :] * padded[
                pl.ds(start + 32 - (n_taps - 1) + k, 128), :
            ]
        conv.append(total)
        sums = jnp.sum(total, axis=1, keepdims=True)
        squares = jnp.sum(total * total, axis=1, keepdims=True)
        both = jnp.where(lane == 0, sums, jnp.where(lane == 1, squares, 0.0))
        stat_out[:, pl.ds(start, 128)] = both.T[:8, :]

    for k in range(1, n_tp):
        remote(
            stat_out, stat_in.at[t], st_send.at[k], st_recv.at[t], {"tp": tp_peer(k)}
        ).start()
    for c in of[3]:
        if c != of[3][0]:
            forward(c, 1)
    each_distance(lambda d: other_halves(of[2], d))
    for k in range(1, n_tp):
        src = tp_peer(k)
        remote(
            stat_out, stat_in.at[src], st_send.at[k], st_recv.at[src], {"tp": src}
        ).wait_recv()
    stats = stat_out[...]
    for k in range(1, n_tp):
        stats = stats + stat_in[tp_peer(k)]
    activated = []
    for i, start in enumerate(range(0, length, 128)):
        turned = jnp.concatenate(
            [stats[:, start : start + 128], jnp.zeros((120, 128), jnp.float32)], axis=0
        ).T
        mean_val = turned[:, 0:1] / total_channels
        mean_sq = turned[:, 1:2] / total_channels
        scaled = (
            (conv[i] - mean_val)
            * lax.rsqrt(mean_sq - mean_val * mean_val + 1e-05)
            * channel_gain[:, mine]
        )
        activated.append(jax.nn.silu(scaled).astype(jnp.bfloat16))
    activated = jnp.concatenate(activated, axis=0)

    def share(part, got, p_send, p_recv, s):
        dest = s // per
        return remote(
            part.at[s], got.at[t, lax.rem(s, per)], p_send.at[s],
            p_recv.at[t, lax.rem(s, per)], {"tp": dest},
        )

    def send_share(part, got, p_send, p_recv, s):
        @pl.when(s // per != t)
        def _():
            share(part, got, p_send, p_recv, s).start()

    def collect(part, got, p_send, p_recv, base, store):
        for k in range(1, n_tp):
            src = tp_peer(k)
            for j in range(per):
                remote(
                    part.at[j], got.at[src, j], p_send.at[j], p_recv.at[src, j], {"tp": src}
                ).wait_recv()
        for j in range(per):
            here = pl.ds(j * rows, rows)
            total = part[t * per + j].astype(jnp.float32)
            for k in range(1, n_tp):
                total = total + got[tp_peer(k), j].astype(jnp.float32)
            store(here, base[here, :].astype(jnp.float32) + total)

    def mix(s, carry):
        part_one[s] = lax.dot_general(
            weight_block(2, s, everything), activated, NT, preferred_element_type=jnp.float32
        ).astype(jnp.bfloat16)
        send_share(part_one, got_one, p1_send, p1_recv, s)
        return carry

    lax.fori_loop(0, n_fs, mix, 0)

    def many(cs, first, last):
        def go(d):
            for c in cs:
                forward(c, d)

        if n_fs <= 4:
            for d in range(first, last):
                go(d)
        else:
            lax.fori_loop(first, last, lambda d, carry: (go(d), carry)[1], 0)

    many(of[3], 2, n_fs - 1)

    def keep_middle(here, value):
        middle_all[0, t, here, :] = value.astype(jnp.bfloat16)

    collect(part_one, got_one, p1_send, p1_recv, x_all.at[t], keep_middle)

    def hand_over(step):
        return remote(
            middle_all.at[0, t], middle_all.at[1, t], g_sem.at[0], g_sem.at[1], {"fs": f + step}
        )

    def spread(g, k):
        block = middle_all.at[g, t]
        return remote(block, block, m_send.at[g, k], m_recv.at[g, t], {"tp": tp_peer(k)})

    @pl.when(jnp.logical_not(inner))
    def _():
        hand_over(toward).start()
        for c in of[5]:
            send_own(c)

    @pl.when(inner)
    def _():
        for k in range(1, n_tp):
            spread(0, k).start()

    many(of[3], n_fs - 1, n_fs)
    for c in of[4]:
        forward(c, 1)

    @pl.when(guest)
    def _():
        hand_over(toward).wait_recv()
        for k in range(1, n_tp):
            spread(1, k).start()

    many(of[4], 2, n_fs - 1)

    def gathered(g):
        for k in range(1, n_tp):
            src = tp_peer(k)
            block = middle_all.at[g, src]
            remote(block, block, m_send.at[g, k], m_recv.at[g, src], {"tp": src}).wait_recv()
        normalize(middle_all.at[g], ffn_gain, g * length)

    units = w3.shape[1]
    tiles = [pl.ds(a, min(256, units - a)) for a in range(0, units, 256)]

    def gates(g):
        for columns in tiles:
            acc[pl.ds(g * length, length), columns] = project(3, columns, g * length)

    def ups(g):
        for columns in tiles:
            here = (pl.ds(g * length, length), columns)
            hidden[here] = (
                jax.nn.silu(acc[here]) * project(4, columns, g * length)
            ).astype(jnp.bfloat16)

    @pl.when(inner)
    def _():
        gathered(0)
        each_distance(lambda d: other_halves(of[3], d))
        for copy in ffn_owns:
            copy.wait()
        gates(0)

    many(of[4], n_fs - 1, n_fs)
    for c in of[5]:
        forward(c, 1)

    @pl.when(guest)
    def _():
        gathered(1)
        gates(1)

    many(of[5], 2, n_fs - 1)

    @pl.when(inner)
    def _():
        each_distance(lambda d: other_halves(of[4], d))
        ups(0)

    @pl.when(guest)
    def _():
        ups(1)

    def sums(g):
        return part_two.at[g], got_two.at[g], p2_send.at[g], p2_recv.at[g]

    def down(s):
        def one(g):
            part_two[g, s] = lax.dot_general(
                bufs[5][s].reshape(rows, units), hidden[pl.ds(g * length, length), :], NT,
                preferred_element_type=jnp.float32,
            ).astype(jnp.bfloat16)
            send_share(*sums(g), s)

        @pl.when(guest)
        def _():
            one(1)

        one(0)

    def down_at(d):
        other_halves(of[5], d)

        def both(i, carry):
            s = f + d - 2 * d * i

            @pl.when(jnp.logical_and(s >= 0, s < n_fs))
            def _():
                down(jnp.clip(s, 0, n_fs - 1))

            return carry

        lax.fori_loop(0, 2, both, 0)

    @pl.when(inner)
    def _():
        down(f)
        if n_fs <= 4:
            for d in range(1, n_fs - 2):
                down_at(d)
        else:
            lax.fori_loop(1, n_fs - 2, lambda d, carry: (down_at(d), carry)[1], 0)

    many(of[5], n_fs - 1, n_fs)

    @pl.when(inner)
    def _():
        down_at(n_fs - 2)

    def give_back(step):
        return remote(returned, back, g_sem.at[2], g_sem.at[3], {"fs": f + step})

    home = jnp.where(f == 1, -1, 1)

    @pl.when(guest)
    def _():
        def keep(here, value):
            returned[here, :] = value.astype(jnp.bfloat16)

        collect(*sums(1), middle_all.at[1, t], keep)
        give_back(home).start()

    @pl.when(inner)
    def _():
        def keep(here, value):
            out[here, :] = value.astype(jnp.bfloat16)

        collect(*sums(0), middle_all.at[0, t], keep)

    @pl.when(jnp.logical_not(inner))
    def _():
        give_back(home).wait_recv()
        out[...] = back[...]

    for copy in x_copies:
        copy.wait_send()
    for k in range(1, n_tp):
        remote(
            stat_out, stat_in.at[t], st_send.at[k], st_recv.at[t], {"tp": tp_peer(k)}
        ).wait_send()

    @pl.when(jnp.logical_not(inner))
    def _():
        hand_over(toward).wait_send()

    @pl.when(inner)
    def _():
        for k in range(1, n_tp):
            spread(0, k).wait_send()

    @pl.when(guest)
    def _():
        for k in range(1, n_tp):
            spread(1, k).wait_send()
        give_back(home).wait_send()

    def drain(s, carry):
        away = s // per != t

        @pl.when(away)
        def _():
            share(part_one, got_one, p1_send, p1_recv, s).wait_send()

        @pl.when(jnp.logical_and(away, inner))
        def _():
            share(*sums(0), s).wait_send()

        @pl.when(jnp.logical_and(away, guest))
        def _():
            share(*sums(1), s).wait_send()

        for c in range(count):
            @pl.when(jnp.logical_and(s <= f, goes_right(c)))
            def _():
                z_copy(c, s, 1).wait_send()

            @pl.when(jnp.logical_and(s >= f, goes_left(c)))
            def _():
                z_copy(c, s, -1).wait_send()

            sent = by_y(c, s)
            if is_ffn(c):
                own_end = jnp.logical_and(s == f, jnp.logical_not(inner))
                sent = jnp.logical_or(sent, own_end)

            @pl.when(sent)
            def _():
                y_copy(c, s, y).wait_send()

        return carry

    lax.fori_loop(0, n_fs, drain, 0)


def on_device(sizes, *args):
    (stream, mixer_gain, glu_value, glu_gate, conv_kernel, channel_gain,
     conv_out, ffn_gain, ffn_gate, ffn_up, ffn_down) = args
    n_grp, n_fs, n_tp = sizes
    weights = (glu_value, glu_gate, conv_out, ffn_gate, ffn_up, ffn_down)
    feats, length = stream.shape
    width = feats * n_tp
    rows = width // n_fs
    channels = glu_value.shape[1]
    units = ffn_gate.shape[1]
    pieces, bufs = [], []
    for w, weight in enumerate(weights):
        subs = 2 if (w >= 3 and n_fs <= 4) else 1
        pieces += [(w, u, subs) for u in range(subs)]
        bufs.append(
            pltpu.VMEM(
                (n_fs, n_grp * subs, rows // (n_grp * subs), weight.shape[1]), jnp.bfloat16
            )
        )
    count = len(pieces)
    per = n_fs // n_tp
    any_spec = pl.BlockSpec(memory_space=pl.ANY)
    vmem = pl.BlockSpec(memory_space=pltpu.VMEM)
    dma = pltpu.SemaphoreType.DMA
    owns = 1 + sum(buf.shape[1] for buf in bufs)
    return pl.pallas_call(
        functools.partial(
            layer_kernel, n_grp, n_fs, n_tp, tuple(pieces), channel_gain.shape[0]
        ),
        out_shape=jax.ShapeDtypeStruct((feats, length), jnp.bfloat16),
        in_specs=[any_spec] * 7 + [vmem] * 4,
        out_specs=vmem,
        scratch_shapes=bufs
        + [
            pltpu.VMEM((n_tp, feats, length), jnp.bfloat16),
            pltpu.VMEM((n_tp, length, feats), jnp.float32),
            pltpu.VMEM((n_fs, 2 * length, rows), jnp.bfloat16),
            pltpu.VMEM((length + 32, channels), jnp.float32),
            pltpu.VMEM((8, length), jnp.float32),
            pltpu.VMEM((n_tp, 8, length), jnp.float32),
            pltpu.VMEM((n_fs, rows, length), jnp.bfloat16),
            pltpu.VMEM((n_tp, per, rows, length), jnp.bfloat16),
            pltpu.VMEM((2, n_tp, feats, length), jnp.bfloat16),
            pltpu.VMEM((2 * length, units), jnp.float32),
            pltpu.VMEM((2 * length, units), jnp.bfloat16),
            pltpu.VMEM((2, n_fs, rows, length), jnp.bfloat16),
            pltpu.VMEM((2, n_tp, per, rows, length), jnp.bfloat16),
            pltpu.VMEM((feats, length), jnp.bfloat16),
            pltpu.VMEM((feats, length), jnp.bfloat16),
        ]
        + [dma((count, n_fs))] * 5
        + [dma((owns,)), dma((4,))]
        + [dma((n_tp,))] * 4
        + [dma((n_tp, per)), dma((n_fs,))]
        + [dma((2, n_tp))] * 2
        + [dma((2, n_tp, per)), dma((2, n_fs))],
        compiler_params=pltpu.CompilerParams(
            collective_id=0, has_side_effects=True, vmem_limit_bytes=62 * 1024 * 1024
        ),
    )(
        stream, *weights, mixer_gain[None, :], conv_kernel, channel_gain[None, :],
        ffn_gain[None, :],
    )


def solution(mesh):
    in_specs = (
        P("tp", ("grp", "fs")),
        P(),
        P("fs", "tp"),
        P("fs", "tp"),
        P(),
        P(),
        P("fs", "tp"),
        P(),
        P("fs", "tp"),
        P("fs", "tp"),
        P("fs", "tp"),
    )
    sizes = (mesh.shape["grp"], mesh.shape["fs"], mesh.shape["tp"])
    return jax.shard_map(
        functools.partial(on_device, sizes), mesh=mesh, in_specs=in_specs,
        out_specs=P("tp", ("grp", "fs")), check_vma=False,
    )
```
